512 devices in a mesh: grp: 2 (over y), sp: 32 (over z), tp: 8 (over x, core).
Axes of the slice: x: 4, y: 2, z: 32, core: 2. Of those that a mesh axis runs over, the one named last changes fastest.
The devices are a block of a 4x8x32 slice.
Arguments:
- tokens: bfloat16 [24576, 2048], P(('grp', 'sp')), parts along dimension 0, may hold values from -6 to 6
- norm_gain: float32 [2048], replicated, may hold values from 0.1 to 1.9
- w_query: bfloat16 [2048, 1024], P(None, 'tp'), may hold values from -0.088388348 to 0.088388348
- w_key: bfloat16 [2048, 1024], P(None, 'tp'), may hold values from -1.5467961 to 1.5467961
- w_value: bfloat16 [2048, 1024], P(None, 'tp'), may hold values from -0.30935922 to 0.30935922
- out_gain: float32 [1024], P('tp'), may hold values from 0.1 to 1.9
- w_out: bfloat16 [1024, 2048], P('tp'), may hold values from -0.1875 to 0.1875
Outputs:
- mixed: bfloat16 [24576, 2048], P(('grp', 'sp', 'tp')), parts along dimension 0
The draws below stay inside these ranges and needn't reach their ends.
There are 2 independent parts, one for each index of `grp`. The reference program is written for one: setup_inputs(seed, part) draws one part's arguments, and reference() takes and returns one part's arrays. A program takes and returns all parts, laid end to end along the dimension named above; an argument that names none is the same for every part. Nothing has to cross between parts.
All inputs are finite; a program needn't handle non-finite values.
Results may differ from the reference program's by a relative error of at most 0.015.
Values may be sent and summed in bfloat16 or wider, within the bound.
No kernel may reach another device: no remote copies, remote signals or barrier semaphores. Data moves between devices by JAX's collectives and lax.ppermute only.
A program may use at most 64 MiB of HBM per device.

```python
from functools import reduce
import jax
import jax.numpy as jnp
from jax import lax

D = 2048
HEADS = 16
HEAD_DIM = 64
WINDOW_FIRST = 128
WINDOW_SECOND = 512
DILATION_SECOND = 4
WINDOW_THIRD = 2048
DILATION_THIRD = 16
SEQ = 12288
WIDTH = 1024
N_TP = 8


def query_raw(key):
    base = jax.random.fold_in(key, 11)
    raw = jnp.clip(jax.random.normal(base, (D, HEADS * HEAD_DIM), jnp.float32), -4.0, 4.0)
    return raw * D ** (-0.5)


def draw_w_query(key, part):
    return query_raw(key).astype(jnp.bfloat16)


def draw_w_key(key, part):
    noise = jnp.clip(jax.random.normal(jax.random.fold_in(key, 23), (D, HEADS * HEAD_DIM), jnp.float32), -4.0, 4.0) * D ** (-0.5)
    result = noise
    return result.astype(jnp.bfloat16)


def draw_w_value(key, part):
    base = jax.random.fold_in(key, 41)
    spread_key = jax.random.fold_in(key, 43)
    raw = jnp.clip(jax.random.normal(base, (D, HEADS * HEAD_DIM), jnp.float32), -4.0, 4.0)
    factors = jnp.exp(jax.random.uniform(spread_key, (HEADS,), jnp.float32, -1.2, 1.2))
    result = raw * D ** (-0.5) * jnp.repeat(factors, HEAD_DIM)[None, :]
    return result.astype(jnp.bfloat16)


def shard_levels(own_key, shape, pieces, low, high):
    gain = 1.0
    for position, shards_of in pieces:
        draws = jax.random.uniform(jax.random.fold_in(jax.random.fold_in(own_key, 6), position), (shards_of,), jnp.float32, low / len(pieces), high / len(pieces))
        gain = gain * jnp.repeat(jnp.exp(draws), shape[position] // shards_of).reshape((-1,) + (1,) * (len(shape) - 1 - position))
    return gain


def normal_values(own_key, dims, width, most, split=(), kind=jnp.bfloat16):
    entries = jax.random.normal(own_key, dims, jnp.float32) * width
    if len(split) > 0:
        entries = shard_levels(own_key, dims, split, -0.22, 0.18) * entries
    return jnp.clip(entries, min=-most, max=most).astype(kind)


def setup_inputs(seed: int = 0, part: int = 0) -> dict:
    key_of = jax.random.split(jax.random.key(seed), 8)
    part_keys = jax.random.split(jax.random.fold_in(key_of[7], part), 8)
    return {
        "tokens": normal_values(part_keys[0], (SEQ, D), 1.0, 6.0, ((0, 32),)),
        "norm_gain": jnp.clip(1.0 + 0.18 * jax.random.normal(key_of[1], (D,), jnp.float32), 0.1, 1.9),
        "w_query": draw_w_query(jax.random.fold_in(key_of[7], 71), part),
        "w_key": draw_w_key(jax.random.fold_in(key_of[7], 71), part),
        "w_value": draw_w_value(jax.random.fold_in(key_of[7], 71), part),
        "out_gain": jnp.clip(1.0 + 0.18 * jax.random.normal(key_of[5], (WIDTH,), jnp.float32), 0.1, 1.9),
        "w_out": normal_values(key_of[6], (WIDTH, D), WIDTH ** -0.5, 0.1875, ((0, 8),)),
    }


EPS = 1e-06
NEG = -1e+30

def band_part(queries, key_rows, value_rows, span_len, dilation_step, first_key):
    query_len, head_count, head_width = queries.shape
    class_len = query_len // dilation_step
    block_len = class_len if class_len <= 128 else 128
    blocks = class_len // block_len
    window_len = block_len + span_len
    query_blk = queries.reshape(blocks, block_len, dilation_step, head_count, head_width)
    key_cls = key_rows.reshape(class_len + span_len, dilation_step, head_count, head_width)
    value_cls = value_rows.reshape(class_len + span_len, dilation_step, head_count, head_width)
    picks = jnp.arange(blocks, dtype=jnp.int32)[:, None] * block_len + jnp.arange(window_len, dtype=jnp.int32)[None, :]
    key_blk = key_cls[picks]
    value_blk = value_cls[picks]
    scores = jnp.einsum('jqchx,jkchx->jchqk', query_blk.astype(jnp.float32), key_blk.astype(jnp.float32)) * HEAD_DIM ** (-0.5)
    lag_steps = span_len + jnp.arange(block_len, dtype=jnp.int32)[:, None] - jnp.arange(window_len, dtype=jnp.int32)[None, :]
    inside = (lag_steps >= 0) & (lag_steps <= span_len)
    key_pos = first_key + (jnp.arange(blocks, dtype=jnp.int32)[:, None, None] * block_len + jnp.arange(window_len, dtype=jnp.int32)[None, None, :]) * dilation_step + jnp.arange(dilation_step, dtype=jnp.int32)[None, :, None]
    usable = inside[None, None, None] & (key_pos >= 0)[:, :, None, None, :]
    scores = jnp.where(usable, scores, NEG)
    row_max = lax.optimization_barrier(jnp.max(scores, axis=-1))
    weights = jnp.exp(scores - row_max[..., None])
    row_sum = lax.optimization_barrier(jnp.sum(weights, axis=-1))
    rounded = lax.optimization_barrier(weights.astype(jnp.bfloat16))
    weighted = jnp.einsum('jchqk,jkchx->jqchx', rounded.astype(jnp.float32), value_blk.astype(jnp.float32))
    weighted = weighted.reshape(query_len, head_count, head_width)
    row_max = jnp.transpose(row_max, (0, 3, 1, 2)).reshape(query_len, head_count)
    row_sum = jnp.transpose(row_sum, (0, 3, 1, 2)).reshape(query_len, head_count)
    return (weighted, row_max, row_sum)

def mixture(pattern_out):
    peak_max = reduce(jnp.maximum, [result[1] for result in pattern_out])
    numerator = reduce(lambda left, right: left + right, [jnp.exp(result[1] - peak_max)[..., None] * result[0] for result in pattern_out])
    denominator = reduce(lambda left, right: left + right, [jnp.exp(result[1] - peak_max) * result[2] for result in pattern_out])
    return numerator / denominator[..., None]

def reference(tokens, norm_gain, w_query, w_key, w_value, out_gain, w_out):
    seq_len = tokens.shape[0]
    tokens_f = tokens.astype(jnp.float32)
    inverse = lax.rsqrt(lax.optimization_barrier(jnp.mean(tokens_f * tokens_f, axis=-1)) + EPS)
    scaled = (tokens_f * norm_gain).astype(jnp.bfloat16)

    def project(weight):
        return (jnp.dot(scaled, weight, preferred_element_type=jnp.float32) * inverse[:, None]).astype(jnp.bfloat16)

    def by_head(matrix):
        return jnp.moveaxis(matrix.reshape(seq_len, HEADS, HEAD_DIM), 1, 0)[:, :, None, :]
    queries = by_head(project(w_query))
    key_rows = by_head(project(w_key))
    value_rows = by_head(project(w_value))
    head_patterns = ((WINDOW_FIRST, 1), (WINDOW_SECOND, DILATION_SECOND), (WINDOW_THIRD, DILATION_THIRD))

    def head_attention(operands):
        head_q, head_k, head_v = operands
        results = []
        for window_span, dilation_step in head_patterns:
            padding = jnp.zeros((window_span, 1, HEAD_DIM), jnp.bfloat16)
            keys_ext = jnp.concatenate([padding, head_k], axis=0)
            values_ext = jnp.concatenate([padding, head_v], axis=0)
            results.append(band_part(head_q, keys_ext, values_ext, window_span // dilation_step, dilation_step, jnp.int32(-window_span)))
        return mixture(results)
    attended = lax.map(head_attention, (queries, key_rows, value_rows))
    attended = jnp.moveaxis(attended[:, :, 0, :], 0, 1).reshape(seq_len, WIDTH)
    out_scale = lax.rsqrt(lax.optimization_barrier(jnp.sum(attended * attended, axis=-1)) / WIDTH + EPS)
    gated = (attended * out_gain).astype(jnp.bfloat16)
    block_w = WIDTH // N_TP

    def add_block(accum, block_idx):
        start_col = (block_idx * block_w).astype(jnp.int32)
        product = jnp.dot(lax.dynamic_slice_in_dim(gated, start_col, block_w, 1), lax.dynamic_slice_in_dim(w_out, start_col, block_w, 0), preferred_element_type=jnp.float32)
        rounded = lax.optimization_barrier(product.astype(jnp.bfloat16))
        return (accum + rounded.astype(jnp.float32), None)
    summed, _ = lax.scan(add_block, jnp.zeros((seq_len, D), jnp.float32), jnp.arange(N_TP, dtype=jnp.int32))
    return (summed * out_scale[:, None]).astype(jnp.bfloat16)
```

```python
import functools

import jax
import jax.numpy as jnp
from jax import lax
from jax.experimental import pallas as pl
from jax.experimental.pallas import tpu as pltpu
from jax.sharding import PartitionSpec as P


HEAD_DIM = 64
WINDOW_FIRST = 128
WINDOW_SECOND = 512
DILATION_SECOND = 4
WINDOW_THIRD = 2048
DILATION_THIRD = 16
CLASSES = DILATION_SECOND

EPS = 1e-06
NEG = -1e30


VMEM = pltpu.VMEM
F32 = jnp.float32
BF16 = jnp.bfloat16


def qkv_kernel(
    chunks, tok_hbm, gain_hbm, wq_hbm, wk_hbm, wv_hbm, q_ref, kv_ref, tok, gain_ref, w, acc, gain_sem, tok_sem, w_sem
):
    rows, depth = tok_hbm.shape
    width = wq_hbm.shape[1]
    piece = depth // chunks
    gain_copy = pltpu.make_async_copy(gain_hbm, gain_ref, gain_sem)
    gain_copy.start()
    copies = []
    for n in range(chunks):
        span = pl.ds(n * piece, piece)
        pair = [pltpu.make_async_copy(tok_hbm.at[:, span], tok.at[:, span], tok_sem.at[n])]
        for m, part in enumerate((wq_hbm, wk_hbm, wv_hbm)):
            pair.append(
                pltpu.make_async_copy(
                    part.at[span, :], w.at[span, pl.ds(m * width, width)], w_sem.at[n, m]
                )
            )
        for copy in pair:
            copy.start()
        copies.append(pair)
    gain_copy.wait()
    squares = jnp.zeros((rows, 128), F32)
    total = jnp.zeros((rows, 3 * width), F32)
    for n in range(chunks):
        for copy in copies[n]:
            copy.wait()
        block = tok[:, n * piece : (n + 1) * piece].astype(F32)
        for lane in range(0, piece, 128):
            part = block[:, lane : lane + 128]
            squares = squares + part * part
        scaled = (block * gain_ref[:, n * piece : (n + 1) * piece]).astype(BF16)
        total = total + jnp.dot(scaled, w[n * piece : (n + 1) * piece, :], preferred_element_type=F32)
    inverse = lax.rsqrt(jnp.sum(squares, axis=-1, keepdims=True) / depth + EPS)
    total = total * inverse
    for m in range(3):
        acc[m] = total[:, m * width : (m + 1) * width]
    share = rows // CLASSES
    for c in range(CLASSES):
        mine = [acc[m, pl.ds(c, share, stride=CLASSES), :] for m in range(3)]
        q_ref[c] = (mine[0] * HEAD_DIM ** (-0.5)).astype(BF16)
        kv_ref[c, :, 0:width] = mine[1].astype(BF16)
        kv_ref[c, :, width : 2 * width] = mine[2].astype(BF16)


def hbm(value):
    return pltpu.with_memory_space_constraint(value, pltpu.HBM)


def qkv(tokens, norm_gain, w_query, w_key, w_value):
    rows, depth = tokens.shape
    width = w_query.shape[1]
    chunks = 4
    share = rows // CLASSES
    return pl.pallas_call(
        functools.partial(qkv_kernel, chunks),
        out_shape=(
            jax.ShapeDtypeStruct((CLASSES, share, width), BF16),
            jax.ShapeDtypeStruct((CLASSES, share, 2 * width), BF16),
        ),
        in_specs=[
            pl.BlockSpec(memory_space=pltpu.HBM),
        ]
        * 5,
        out_specs=(pl.BlockSpec(memory_space=VMEM), pl.BlockSpec(memory_space=VMEM)),
        scratch_shapes=[
            VMEM((rows, depth), BF16),
            VMEM((1, depth), F32),
            VMEM((depth, 3 * width), BF16),
            VMEM((3, rows, width), F32),
            pltpu.SemaphoreType.DMA,
            pltpu.SemaphoreType.DMA((chunks,)),
            pltpu.SemaphoreType.DMA((chunks, 3)),
        ],
        compiler_params=pltpu.CompilerParams(vmem_limit_bytes=20 << 20),
        name="qkv",
    )(hbm(tokens), hbm(norm_gain.reshape(1, depth)), hbm(w_query), hbm(w_key), hbm(w_value))


def attend_kernel(sp_ref, q_ref, own, *rest):
    older = rest[:-4]
    out_ref, k_all, v_all, natural = rest[-4:]
    width = q_ref.shape[2]
    share = q_ref.shape[1]
    far = WINDOW_THIRD // CLASSES
    near = WINDOW_FIRST // CLASSES
    span = far + share
    tail = near + share
    start = span
    for block in (own, *older):
        count = block.shape[1]
        start -= count
        for c in range(CLASSES):
            k_all[c, start : start + count, :] = block[c, :, 0:width]
            v_all[c, start : start + count, :] = block[c, :, width : 2 * width]
    sp = sp_ref[0]
    row = lax.broadcasted_iota(jnp.int32, (share, span), 0)
    col = lax.broadcasted_iota(jnp.int32, (share, span), 1)
    lag = row - col + far
    ratio = DILATION_THIRD // CLASSES
    behind = (lag >= 0).astype(F32)
    count = behind * (
        (lag <= WINDOW_FIRST // CLASSES).astype(F32)
        + (lag <= WINDOW_SECOND // CLASSES).astype(F32)
        + jnp.logical_and(lag <= far, lax.rem(lag + ratio * span, ratio) == 0).astype(F32)
    )
    live = jnp.logical_and(count > 0.5, col >= far - share * sp)
    weight = jnp.where(count > 2.5, jnp.log(F32(3.0)), jnp.where(count > 1.5, jnp.log(F32(2.0)), F32(0.0)))
    bias = jnp.where(live, weight, NEG)
    bias = jnp.concatenate([bias, bias], axis=0)
    row = lax.broadcasted_iota(jnp.int32, (share, tail), 0)
    col = lax.broadcasted_iota(jnp.int32, (share, tail), 1)
    lag = row - col + near
    there = col >= near - share * sp
    after = jnp.where(jnp.logical_and(there, jnp.logical_and(lag >= 0, lag < near)), F32(0.0), NEG)
    before = jnp.where(jnp.logical_and(there, jnp.logical_and(lag >= 1, lag <= near)), F32(0.0), NEG)
    after = jnp.concatenate([after, after], axis=0)
    before = jnp.concatenate([before, before], axis=0)
    lane = lax.broadcasted_iota(jnp.int32, (share, width), 1)
    contract = (((1,), (1,)), ((), ()))
    for c in range(CLASSES):
        query = q_ref[c]
        zero = jnp.zeros_like(query)
        stacked = jnp.concatenate(
            [jnp.where(lane < HEAD_DIM, query, zero), jnp.where(lane < HEAD_DIM, zero, query)], axis=0
        )
        scores = [lax.dot_general(stacked, k_all[c], contract, preferred_element_type=F32) + bias]
        values = [v_all[c]]
        for other in range(CLASSES):
            if other != c:
                part = lax.dot_general(
                    stacked, k_all[other, span - tail : span, :], contract, preferred_element_type=F32
                )
                scores.append(part + (after if c > other else before))
                values.append(v_all[other, span - tail : span, :])
        top = functools.reduce(jnp.maximum, [jnp.max(part, axis=-1, keepdims=True) for part in scores])
        weights = [jnp.exp(part - top) for part in scores]
        norm = functools.reduce(jnp.add, [jnp.sum(part, axis=-1, keepdims=True) for part in weights])
        mixed = functools.reduce(
            jnp.add,
            [
                jnp.dot(part.astype(BF16), value, preferred_element_type=F32)
                for part, value in zip(weights, values)
            ],
        )
        mixed = mixed / norm
        natural[pl.ds(c, share, stride=CLASSES), :] = jnp.where(lane < HEAD_DIM, mixed[:share], mixed[share:])
    out_ref[...] = natural[...].astype(BF16)


def attend(sp, query, own, older):
    share, width = query.shape[1:]
    span = WINDOW_THIRD // CLASSES + share
    return pl.pallas_call(
        attend_kernel,
        out_shape=jax.ShapeDtypeStruct((CLASSES * share, width), BF16),
        in_specs=[pl.BlockSpec(memory_space=pltpu.SMEM)]
        + [pl.BlockSpec(memory_space=VMEM)] * (2 + len(older)),
        out_specs=pl.BlockSpec(memory_space=VMEM),
        scratch_shapes=[
            VMEM((CLASSES, span, width), BF16),
            VMEM((CLASSES, span, width), BF16),
            VMEM((CLASSES * share, width), F32),
        ],
        compiler_params=pltpu.CompilerParams(vmem_limit_bytes=20 << 20),
        name="attend",
    )(sp, query, own, *older)


def project_kernel(tp_ref, att_ref, mine, partner, out_ref):
    count, rows, width = att_ref.shape
    tp = tp_ref[0]
    squares = jnp.zeros((rows, width), F32)
    for n in range(count):
        part = att_ref[n].astype(F32)
        squares = squares + part * part
    scale = lax.rsqrt(jnp.sum(squares, axis=-1, keepdims=True) / (count * width) + EPS)
    total = None
    for other, weights in ((0, mine), (1, partner)):
        places = [lax.rem(lax.bitwise_xor(tp, other) + step + count, count) for step in (0, -2, 2, 4)]
        left = jnp.concatenate([att_ref[place] for place in places], axis=1)
        part = jnp.dot(left, weights[...], preferred_element_type=F32)
        total = part if total is None else total + part
    out_ref[...] = (total * scale).astype(BF16)


def project(tp, attended, mine, partner):
    rows = attended.shape[1]
    return pl.pallas_call(
        project_kernel,
        out_shape=jax.ShapeDtypeStruct((rows, mine.shape[1]), BF16),
        in_specs=[pl.BlockSpec(memory_space=pltpu.SMEM)] + [pl.BlockSpec(memory_space=VMEM)] * 3,
        out_specs=pl.BlockSpec(memory_space=VMEM),
        compiler_params=pltpu.CompilerParams(vmem_limit_bytes=20 << 20),
        name="project",
    )(tp, attended, mine, partner)


def ahead(value, steps, first):
    count = lax.axis_size("sp")
    return lax.ppermute(value, "sp", [(source, source + steps) for source in range(first, count - steps)])


def across(value, pairs):
    return lax.ppermute(value, "tp", pairs)


def layer(tokens, norm_gain, w_query, w_key, w_value, out_gain, w_out):
    tok_rows = tokens.shape[0]
    sp = lax.axis_index("sp").astype(jnp.int32).reshape(1)
    tp = lax.axis_index("tp").astype(jnp.int32).reshape(1)
    n_tp = lax.axis_size("tp")
    query, own = qkv(tokens, norm_gain, w_query, w_key, w_value)

    one = ahead(own, 1, 0)
    two = ahead(own, 2, 0)
    three = ahead(one, 2, 1)
    four = ahead(two, 2, 2)
    five = ahead(three, 2, 3)
    excess = 6 * (tok_rows // CLASSES) - WINDOW_THIRD // CLASSES
    six = ahead(four[:, excess:, :], 2, 4)

    scaled_out = (w_out.astype(F32) * out_gain[:, None]).astype(BF16)
    up = [(n, (n + 2) % n_tp) for n in range(n_tp)]
    down = [(n, (n - 2) % n_tp) for n in range(n_tp)]
    swap = [(n, n ^ 1) for n in range(n_tp)]
    half = w_out.shape[0] // 2
    behind = across(scaled_out, up)
    front = across(scaled_out, down)
    far_low = across(behind[:half], up)
    far_high = across(front[half:], down)
    mine = jnp.concatenate([scaled_out, behind, front, far_low, far_high], axis=0)
    partner = across(mine, swap)

    attended = attend(sp, query, own, (one, two, three, four, five, six))
    tiles = attended.reshape(n_tp, tok_rows // n_tp, -1)
    arrived = lax.all_to_all(tiles, "tp", split_axis=0, concat_axis=0, tiled=True)
    return project(tp, arrived, mine, partner)


def solution(mesh):
    in_specs = (
        P(("grp", "sp"), None),
        P(),
        P(None, "tp"),
        P(None, "tp"),
        P(None, "tp"),
        P("tp"),
        P("tp", None),
    )
    out_specs = P(("grp", "sp", "tp"), None)
    return jax.shard_map(layer, mesh=mesh, in_specs=in_specs, out_specs=out_specs, check_vma=False)
```

```python
import functools

import jax
import jax.numpy as jnp
from jax import lax
from jax.experimental import pallas as pl
from jax.experimental.pallas import tpu as pltpu
from jax.sharding import PartitionSpec as P


HEAD_DIM = 64
WINDOW_FIRST = 128
WINDOW_SECOND = 512
DILATION_SECOND = 4
WINDOW_THIRD = 2048
DILATION_THIRD = 16
CLASSES = DILATION_SECOND

EPS = 1e-06
NEG = -1e30


VMEM = pltpu.VMEM
F32 = jnp.float32
BF16 = jnp.bfloat16


def qkv_kernel(
    chunks, tok_hbm, gain_hbm, wq_hbm, wk_hbm, wv_hbm, q_ref, kv_ref, tok, gain_ref, w, acc, gain_sem, tok_sem, w_sem
):
    rows, depth = tok_hbm.shape
    width = wq_hbm.shape[1]
    piece = depth // chunks
    gain_copy = pltpu.make_async_copy(gain_hbm, gain_ref, gain_sem)
    gain_copy.start()
    copies = []
    for n in range(chunks):
        span = pl.ds(n * piece, piece)
        pair = [pltpu.make_async_copy(tok_hbm.at[:, span], tok.at[:, span], tok_sem.at[n])]
        for m, part in enumerate((wq_hbm, wk_hbm, wv_hbm)):
            pair.append(
                pltpu.make_async_copy(
                    part.at[span, :], w.at[span, pl.ds(m * width, width)], w_sem.at[n, m]
                )
            )
        for copy in pair:
            copy.start()
        copies.append(pair)
    gain_copy.wait()
    squares = jnp.zeros((rows, 128), F32)
    total = jnp.zeros((rows, 3 * width), F32)
    for n in range(chunks):
        for copy in copies[n]:
            copy.wait()
        block = tok[:, n * piece : (n + 1) * piece].astype(F32)
        for lane in range(0, piece, 128):
            part = block[:, lane : lane + 128]
            squares = squares + part * part
        scaled = (block * gain_ref[:, n * piece : (n + 1) * piece]).astype(BF16)
        total = total + jnp.dot(scaled, w[n * piece : (n + 1) * piece, :], preferred_element_type=F32)
    inverse = lax.rsqrt(jnp.sum(squares, axis=-1, keepdims=True) / depth + EPS)
    total = total * inverse
    for m in range(3):
        acc[m] = total[:, m * width : (m + 1) * width]
    share = rows // CLASSES
    for c in range(CLASSES):
        mine = [acc[m, pl.ds(c, share, stride=CLASSES), :] for m in range(3)]
        q_ref[c] = (mine[0] * HEAD_DIM ** (-0.5)).astype(BF16)
        kv_ref[c, :, 0:width] = mine[1].astype(BF16)
        kv_ref[c, :, width : 2 * width] = mine[2].astype(BF16)


def hbm(value):
    return pltpu.with_memory_space_constraint(value, pltpu.HBM)


def qkv(tokens, norm_gain, w_query, w_key, w_value):
    rows, depth = tokens.shape
    width = w_query.shape[1]
    chunks = 4
    share = rows // CLASSES
    return pl.pallas_call(
        functools.partial(qkv_kernel, chunks),
        out_shape=(
            jax.ShapeDtypeStruct((CLASSES, share, width), BF16),
            jax.ShapeDtypeStruct((CLASSES, share, 2 * width), BF16),
        ),
        in_specs=[
            pl.BlockSpec(memory_space=pltpu.HBM),
        ]
        * 5,
        out_specs=(pl.BlockSpec(memory_space=VMEM), pl.BlockSpec(memory_space=VMEM)),
        scratch_shapes=[
            VMEM((rows, depth), BF16),
            VMEM((1, depth), F32),
            VMEM((depth, 3 * width), BF16),
            VMEM((3, rows, width), F32),
            pltpu.SemaphoreType.DMA,
            pltpu.SemaphoreType.DMA((chunks,)),
            pltpu.SemaphoreType.DMA((chunks, 3)),
        ],
        compiler_params=pltpu.CompilerParams(vmem_limit_bytes=20 << 20),
        name="qkv",
    )(hbm(tokens), hbm(norm_gain.reshape(1, depth)), hbm(w_query), hbm(w_key), hbm(w_value))


def split(value, lanes):
    high = value.astype(BF16)
    left = value - high.astype(F32)
    middle = left.astype(BF16)
    low = (left - middle.astype(F32)).astype(BF16)
    lane = lax.broadcasted_iota(jnp.int32, (value.shape[0], lanes), 1)
    zero = jnp.zeros((value.shape[0], lanes), F32)
    spread = jnp.where(lane == 0, high.astype(F32), jnp.where(lane == 1, middle.astype(F32), jnp.where(lane == 2, low.astype(F32), zero)))
    return spread.astype(BF16)


def attend_kernel(sp_ref, core_ref, q_ref, own, *rest):
    older = rest[:-6]
    gain_ref, keep_ref, give_ref, k_all, v_all, natural = rest[-6:]
    width = q_ref.shape[2]
    share = q_ref.shape[1]
    far = WINDOW_THIRD // CLASSES
    near = WINDOW_FIRST // CLASSES
    span = far + share
    tail = near + share
    start = span
    for block in (own, *older):
        count = block.shape[1]
        start -= count
        for c in range(CLASSES):
            k_all[c, start : start + count, :] = block[c, :, 0:width]
            v_all[c, start : start + count, :] = block[c, :, width : 2 * width]
    sp = sp_ref[0]
    row = lax.broadcasted_iota(jnp.int32, (share, span), 0)
    col = lax.broadcasted_iota(jnp.int32, (share, span), 1)
    lag = row - col + far
    ratio = DILATION_THIRD // CLASSES
    behind = (lag >= 0).astype(F32)
    count = behind * (
        (lag <= WINDOW_FIRST // CLASSES).astype(F32)
        + (lag <= WINDOW_SECOND // CLASSES).astype(F32)
        + jnp.logical_and(lag <= far, lax.rem(lag + ratio * span, ratio) == 0).astype(F32)
    )
    live = jnp.logical_and(count > 0.5, col >= far - share * sp)
    weight = jnp.where(count > 2.5, jnp.log(F32(3.0)), jnp.where(count > 1.5, jnp.log(F32(2.0)), F32(0.0)))
    bias = jnp.where(live, weight, NEG)
    bias = jnp.concatenate([bias, bias], axis=0)
    row = lax.broadcasted_iota(jnp.int32, (share, tail), 0)
    col = lax.broadcasted_iota(jnp.int32, (share, tail), 1)
    lag = row - col + near
    there = col >= near - share * sp
    after = jnp.where(jnp.logical_and(there, jnp.logical_and(lag >= 0, lag < near)), F32(0.0), NEG)
    before = jnp.where(jnp.logical_and(there, jnp.logical_and(lag >= 1, lag <= near)), F32(0.0), NEG)
    after = jnp.concatenate([after, after], axis=0)
    before = jnp.concatenate([before, before], axis=0)
    lane = lax.broadcasted_iota(jnp.int32, (share, width), 1)
    contract = (((1,), (1,)), ((), ()))
    for c in range(CLASSES):
        query = q_ref[c]
        zero = jnp.zeros_like(query)
        stacked = jnp.concatenate(
            [jnp.where(lane < HEAD_DIM, query, zero), jnp.where(lane < HEAD_DIM, zero, query)], axis=0
        )
        scores = [lax.dot_general(stacked, k_all[c], contract, preferred_element_type=F32) + bias]
        values = [v_all[c]]
        for other in range(CLASSES):
            if other != c:
                part = lax.dot_general(
                    stacked, k_all[other, span - tail : span, :], contract, preferred_element_type=F32
                )
                scores.append(part + (after if c > other else before))
                values.append(v_all[other, span - tail : span, :])
        top = functools.reduce(jnp.maximum, [jnp.max(part, axis=-1, keepdims=True) for part in scores])
        weights = [jnp.exp(part - top) for part in scores]
        norm = functools.reduce(jnp.add, [jnp.sum(part, axis=-1, keepdims=True) for part in weights])
        mixed = functools.reduce(
            jnp.add,
            [
                jnp.dot(part.astype(BF16), value, preferred_element_type=F32)
                for part, value in zip(weights, values)
            ],
        )
        mixed = mixed / norm
        natural[pl.ds(c, share, stride=CLASSES), :] = jnp.where(lane < HEAD_DIM, mixed[:share], mixed[share:])
    core = core_ref[0]
    part = keep_ref.shape[1]
    for side, target in ((core, keep_ref), (1 - core, give_ref)):
        for place in range(keep_ref.shape[0]):
            first = pl.multiple_of((2 * place + side) * part, 16)
            block = natural[pl.ds(first, part), :]
            target[place, :, 0:width] = (block * gain_ref[...]).astype(BF16)
            target[place, :, width : 2 * width] = split(jnp.sum(block * block, axis=-1, keepdims=True), width)


def attend(sp, core, query, own, older, gain, parts):
    share, width = query.shape[1:]
    span = WINDOW_THIRD // CLASSES + share
    return pl.pallas_call(
        attend_kernel,
        out_shape=(jax.ShapeDtypeStruct((parts, CLASSES * share // (2 * parts), 2 * width), BF16),) * 2,
        in_specs=[pl.BlockSpec(memory_space=pltpu.SMEM)] * 2
        + [pl.BlockSpec(memory_space=VMEM)] * (3 + len(older)),
        out_specs=(pl.BlockSpec(memory_space=VMEM),) * 2,
        scratch_shapes=[
            VMEM((CLASSES, span, width), BF16),
            VMEM((CLASSES, span, width), BF16),
            VMEM((CLASSES * share, width), F32),
        ],
        compiler_params=pltpu.CompilerParams(vmem_limit_bytes=20 << 20),
        name="attend",
    )(sp, core, query, own, *older, gain)


def product_kernel(keep_ref, got_ref, mine, partner, out_ref):
    parts, rows, double = keep_ref.shape
    width = double // 2
    columns = mine.shape[1]
    keep = keep_ref[...].reshape(parts * rows, double)
    got = got_ref[...].reshape(parts * rows, double)
    total = jnp.dot(keep[:, :width], mine[...], preferred_element_type=F32)
    total = total + jnp.dot(got[:, :width], partner[...], preferred_element_type=F32)
    squares = jnp.sum(keep[:, width:].astype(F32) + got[:, width:].astype(F32), axis=-1, keepdims=True)
    out_ref[:, :, 0:columns] = total.astype(BF16).reshape(parts, rows, columns)
    out_ref[:, :, columns : columns + width] = split(squares, width).reshape(parts, rows, width)


def product(keep, got, mine, partner):
    parts, rows, double = keep.shape
    return pl.pallas_call(
        product_kernel,
        out_shape=jax.ShapeDtypeStruct((parts, rows, mine.shape[1] + double // 2), BF16),
        in_specs=[pl.BlockSpec(memory_space=VMEM)] * 4,
        out_specs=pl.BlockSpec(memory_space=VMEM),
        compiler_params=pltpu.CompilerParams(vmem_limit_bytes=20 << 20),
        name="product",
    )(keep, got, mine, partner)


def finish_kernel(channels, parts_ref, out_ref):
    parts, rows, columns = parts_ref.shape
    wide = out_ref.shape[1]
    squares = jnp.zeros((rows, columns - wide), F32)
    for n in range(parts):
        squares = squares + parts_ref[n, :, wide:columns].astype(F32)
    scale = lax.rsqrt(jnp.sum(squares, axis=-1, keepdims=True) / channels + EPS)
    total = parts_ref[0, :, 0:wide].astype(F32)
    for n in range(1, parts):
        total = total + parts_ref[n, :, 0:wide].astype(F32)
    out_ref[...] = (total * scale).astype(BF16)


def finish(arrived, wide, channels):
    return pl.pallas_call(
        functools.partial(finish_kernel, channels),
        out_shape=jax.ShapeDtypeStruct((arrived.shape[1], wide), BF16),
        in_specs=[pl.BlockSpec(memory_space=VMEM)],
        out_specs=pl.BlockSpec(memory_space=VMEM),
        compiler_params=pltpu.CompilerParams(vmem_limit_bytes=20 << 20),
        name="finish",
    )(arrived)


def ahead(value, steps, first):
    count = lax.axis_size("sp")
    return lax.ppermute(value, "sp", [(source, source + steps) for source in range(first, count - steps)])


def across(value, pairs):
    return lax.ppermute(value, "tp", pairs)


def layer(tokens, norm_gain, w_query, w_key, w_value, out_gain, w_out):
    tok_rows = tokens.shape[0]
    sp = lax.axis_index("sp").astype(jnp.int32).reshape(1)
    tp = lax.axis_index("tp").astype(jnp.int32).reshape(1)
    n_tp = lax.axis_size("tp")
    query, own = qkv(tokens, norm_gain, w_query, w_key, w_value)

    one = ahead(own, 1, 0)
    two = ahead(own, 2, 0)
    three = ahead(one, 2, 1)
    four = ahead(two, 2, 2)
    five = ahead(three, 2, 3)
    excess = 6 * (tok_rows // CLASSES) - WINDOW_THIRD // CLASSES
    six = ahead(four[:, excess:, :], 2, 4)

    swap = [(n, n ^ 1) for n in range(n_tp)]
    same_core = [list(range(core, n_tp, 2)) for core in range(2)]
    partner = across(w_out, swap)
    keep, give = attend(
        sp, lax.rem(tp, 2), query, own, (one, two, three, four, five, six), out_gain.reshape(1, -1), n_tp // 2
    )
    got = across(give, swap)
    tiles = product(keep, got, w_out, partner)
    arrived = lax.all_to_all(tiles, "tp", split_axis=0, concat_axis=0, axis_index_groups=same_core, tiled=True)
    return finish(arrived, w_out.shape[1], n_tp * w_out.shape[0])


def solution(mesh):
    in_specs = (
        P(("grp", "sp"), None),
        P(),
        P(None, "tp"),
        P(None, "tp"),
        P(None, "tp"),
        P("tp"),
        P("tp", None),
    )
    out_specs = P(("grp", "sp", "tp"), None)
    return jax.shard_map(layer, mesh=mesh, in_specs=in_specs, out_specs=out_specs, check_vma=False)
```

```python
import functools

import jax
import jax.numpy as jnp
from jax import lax
from jax.experimental import pallas as pl
from jax.experimental.pallas import tpu as pltpu
from jax.sharding import PartitionSpec as P


HEAD_DIM = 64
WINDOW_FIRST = 128
WINDOW_SECOND = 512
DILATION_SECOND = 4
WINDOW_THIRD = 2048
DILATION_THIRD = 16
CLASSES = DILATION_SECOND

EPS = 1e-06
NEG = -1e30


VMEM = pltpu.VMEM
F32 = jnp.float32
BF16 = jnp.bfloat16


def qkv_kernel(
    chunks, tok_hbm, gain_hbm, wq_hbm, wk_hbm, wv_hbm, q_ref, kv_ref, tok, gain_ref, w, acc, gain_sem, tok_sem, w_sem
):
    rows, depth = tok_hbm.shape
    width = wq_hbm.shape[1]
    piece = depth // chunks
    gain_copy = pltpu.make_async_copy(gain_hbm, gain_ref, gain_sem)
    gain_copy.start()
    copies = []
    for n in range(chunks):
        span = pl.ds(n * piece, piece)
        pair = [pltpu.make_async_copy(tok_hbm.at[:, span], tok.at[:, span], tok_sem.at[n])]
        for m, part in enumerate((wq_hbm, wk_hbm, wv_hbm)):
            pair.append(
                pltpu.make_async_copy(
                    part.at[span, :], w.at[span, pl.ds(m * width, width)], w_sem.at[n, m]
                )
            )
        for copy in pair:
            copy.start()
        copies.append(pair)
    gain_copy.wait()
    squares = jnp.zeros((rows, 128), F32)
    total = jnp.zeros((rows, 3 * width), F32)
    for n in range(chunks):
        for copy in copies[n]:
            copy.wait()
        block = tok[:, n * piece : (n + 1) * piece].astype(F32)
        for lane in range(0, piece, 128):
            part = block[:, lane : lane + 128]
            squares = squares + part * part
        scaled = (block * gain_ref[:, n * piece : (n + 1) * piece]).astype(BF16)
        total = total + jnp.dot(scaled, w[n * piece : (n + 1) * piece, :], preferred_element_type=F32)
    inverse = lax.rsqrt(jnp.sum(squares, axis=-1, keepdims=True) / depth + EPS)
    total = total * inverse
    for m in range(3):
        acc[m] = total[:, m * width : (m + 1) * width]
    share = rows // CLASSES
    for c in range(CLASSES):
        mine = [acc[m, pl.ds(c, share, stride=CLASSES), :] for m in range(3)]
        q_ref[c] = (mine[0] * HEAD_DIM ** (-0.5)).astype(BF16)
        kv_ref[c, :, 0:width] = mine[1].astype(BF16)
        kv_ref[c, :, width : 2 * width] = mine[2].astype(BF16)


def hbm(value):
    return pltpu.with_memory_space_constraint(value, pltpu.HBM)


def qkv(tokens, norm_gain, w_query, w_key, w_value):
    rows, depth = tokens.shape
    width = w_query.shape[1]
    chunks = 4
    share = rows // CLASSES
    return pl.pallas_call(
        functools.partial(qkv_kernel, chunks),
        out_shape=(
            jax.ShapeDtypeStruct((CLASSES, share, width), BF16),
            jax.ShapeDtypeStruct((CLASSES, share, 2 * width), BF16),
        ),
        in_specs=[
            pl.BlockSpec(memory_space=pltpu.HBM),
        ]
        * 5,
        out_specs=(pl.BlockSpec(memory_space=VMEM), pl.BlockSpec(memory_space=VMEM)),
        scratch_shapes=[
            VMEM((rows, depth), BF16),
            VMEM((1, depth), F32),
            VMEM((depth, 3 * width), BF16),
            VMEM((3, rows, width), F32),
            pltpu.SemaphoreType.DMA,
            pltpu.SemaphoreType.DMA((chunks,)),
            pltpu.SemaphoreType.DMA((chunks, 3)),
        ],
        compiler_params=pltpu.CompilerParams(vmem_limit_bytes=20 << 20),
        name="qkv",
    )(hbm(tokens), hbm(norm_gain.reshape(1, depth)), hbm(w_query), hbm(w_key), hbm(w_value))


def split(value, lanes):
    high = value.astype(BF16)
    left = value - high.astype(F32)
    middle = left.astype(BF16)
    low = (left - middle.astype(F32)).astype(BF16)
    lane = lax.broadcasted_iota(jnp.int32, (value.shape[0], lanes), 1)
    zero = jnp.zeros((value.shape[0], lanes), F32)
    spread = jnp.where(lane == 0, high.astype(F32), jnp.where(lane == 1, middle.astype(F32), jnp.where(lane == 2, low.astype(F32), zero)))
    return spread.astype(BF16)


def both_heads(query, lane):
    zero = jnp.zeros_like(query)
    return jnp.concatenate([jnp.where(lane < HEAD_DIM, query, zero), jnp.where(lane < HEAD_DIM, zero, query)], axis=0)


def twice(value):
    return jnp.concatenate([value, value], axis=0)


def third_hit(lag):
    ratio = DILATION_THIRD // CLASSES
    reach = WINDOW_THIRD // CLASSES
    return jnp.logical_and(lag <= reach, lax.rem(lag, ratio) == 0)


CONTRACT = (((1,), (1,)), ((), ()))


def near_kernel(sp_ref, q_ref, own, *rest):
    older = rest[:-5]
    top_ref, norm_ref, sum_ref, k_all, v_all = rest[-5:]
    share, width = q_ref.shape[1:]
    span = k_all.shape[1]
    far = span - share
    near = WINDOW_FIRST // CLASSES
    tail = near + share
    start = span
    for block in (own, *older):
        start -= share
        for c in range(CLASSES):
            k_all[c, start : start + share, :] = block[c, :, 0:width]
            v_all[c, start : start + share, :] = block[c, :, width : 2 * width]
    sp = sp_ref[0]
    row = lax.broadcasted_iota(jnp.int32, (share, span), 0)
    col = lax.broadcasted_iota(jnp.int32, (share, span), 1)
    lag = row - col + far
    behind = lag >= 0
    lag = jnp.maximum(lag, 0)
    count = (
        (lag <= WINDOW_FIRST // CLASSES).astype(F32)
        + (lag <= WINDOW_SECOND // CLASSES).astype(F32)
        + third_hit(lag).astype(F32)
    )
    live = jnp.logical_and(jnp.logical_and(behind, count > 0.5), col >= far - share * sp)
    weight = jnp.where(count > 2.5, jnp.log(F32(3.0)), jnp.where(count > 1.5, jnp.log(F32(2.0)), F32(0.0)))
    bias = twice(jnp.where(live, weight, NEG))
    row = lax.broadcasted_iota(jnp.int32, (share, tail), 0)
    col = lax.broadcasted_iota(jnp.int32, (share, tail), 1)
    lag = row - col + near
    there = col >= near - share * sp
    after = twice(jnp.where(jnp.logical_and(there, jnp.logical_and(lag >= 0, lag < near)), F32(0.0), NEG))
    before = twice(jnp.where(jnp.logical_and(there, jnp.logical_and(lag >= 1, lag <= near)), F32(0.0), NEG))
    lane = lax.broadcasted_iota(jnp.int32, (share, width), 1)
    for c in range(CLASSES):
        stacked = both_heads(q_ref[c], lane)
        scores = [lax.dot_general(stacked, k_all[c], CONTRACT, preferred_element_type=F32) + bias]
        values = [v_all[c]]
        for other in range(CLASSES):
            if other != c:
                part = lax.dot_general(
                    stacked, k_all[other, span - tail : span, :], CONTRACT, preferred_element_type=F32
                )
                scores.append(part + (after if c > other else before))
                values.append(v_all[other, span - tail : span, :])
        top = functools.reduce(jnp.maximum, [jnp.max(part, axis=-1, keepdims=True) for part in scores])
        weights = [jnp.exp(part - top) for part in scores]
        top_ref[c] = top
        norm_ref[c] = functools.reduce(jnp.add, [jnp.sum(part, axis=-1, keepdims=True) for part in weights])
        sum_ref[c] = functools.reduce(
            jnp.add,
            [
                jnp.dot(part.astype(BF16), value, preferred_element_type=F32)
                for part, value in zip(weights, values)
            ],
        )


def attend_near(sp, query, own, older):
    share, width = query.shape[1:]
    span = (1 + len(older)) * share
    return pl.pallas_call(
        near_kernel,
        out_shape=(
            jax.ShapeDtypeStruct((CLASSES, 2 * share, 1), F32),
            jax.ShapeDtypeStruct((CLASSES, 2 * share, 1), F32),
            jax.ShapeDtypeStruct((CLASSES, 2 * share, width), F32),
        ),
        in_specs=[pl.BlockSpec(memory_space=pltpu.SMEM)]
        + [pl.BlockSpec(memory_space=VMEM)] * (2 + len(older)),
        out_specs=(pl.BlockSpec(memory_space=VMEM),) * 3,
        scratch_shapes=[VMEM((CLASSES, span, width), BF16), VMEM((CLASSES, span, width), BF16)],
        compiler_params=pltpu.CompilerParams(vmem_limit_bytes=20 << 20),
        name="attend_near",
    )(sp, query, own, *older)


def far_kernel(sp_ref, core_ref, q_ref, five, six, top_ref, norm_ref, sum_ref, gain_ref, keep_ref, give_ref, natural):
    share, width = q_ref.shape[1:]
    count = five.shape[1] + six.shape[1]
    far = WINDOW_THIRD // CLASSES
    row = lax.broadcasted_iota(jnp.int32, (share, count), 0)
    col = lax.broadcasted_iota(jnp.int32, (share, count), 1)
    live = jnp.logical_and(third_hit(row - col + far), col >= far - share * sp_ref[0])
    bias = twice(jnp.where(live, F32(0.0), NEG))
    lane = lax.broadcasted_iota(jnp.int32, (share, width), 1)
    for c in range(CLASSES):
        stacked = both_heads(q_ref[c], lane)
        keys = jnp.concatenate([six[c, :, 0:width], five[c, :, 0:width]], axis=0)
        values = jnp.concatenate([six[c, :, width : 2 * width], five[c, :, width : 2 * width]], axis=0)
        score = lax.dot_general(stacked, keys, CONTRACT, preferred_element_type=F32) + bias
        top = jnp.maximum(top_ref[c], jnp.max(score, axis=-1, keepdims=True))
        shrink = jnp.exp(top_ref[c] - top)
        weight = jnp.exp(score - top)
        norm = norm_ref[c] * shrink + jnp.sum(weight, axis=-1, keepdims=True)
        mixed = sum_ref[c] * shrink + jnp.dot(weight.astype(BF16), values, preferred_element_type=F32)
        mixed = mixed / norm
        natural[pl.ds(c, share, stride=CLASSES), :] = jnp.where(lane < HEAD_DIM, mixed[:share], mixed[share:])
    core = core_ref[0]
    part = keep_ref.shape[1]
    for side, target in ((core, keep_ref), (1 - core, give_ref)):
        for place in range(keep_ref.shape[0]):
            first = pl.multiple_of((2 * place + side) * part, 16)
            block = natural[pl.ds(first, part), :]
            target[place, :, 0:width] = (block * gain_ref[...]).astype(BF16)
            target[place, :, width : 2 * width] = split(jnp.sum(block * block, axis=-1, keepdims=True), width)


def attend_far(sp, core, query, five, six, state, gain, parts):
    share, width = query.shape[1:]
    return pl.pallas_call(
        far_kernel,
        out_shape=(jax.ShapeDtypeStruct((parts, CLASSES * share // (2 * parts), 2 * width), BF16),) * 2,
        in_specs=[pl.BlockSpec(memory_space=pltpu.SMEM)] * 2 + [pl.BlockSpec(memory_space=VMEM)] * 7,
        out_specs=(pl.BlockSpec(memory_space=VMEM),) * 2,
        scratch_shapes=[VMEM((CLASSES * share, width), F32)],
        compiler_params=pltpu.CompilerParams(vmem_limit_bytes=20 << 20),
        name="attend_far",
    )(sp, core, query, five, six, *state, gain)


def product_kernel(keep_ref, got_ref, mine, partner, out_ref):
    parts, rows, double = keep_ref.shape
    width = double // 2
    columns = mine.shape[1]
    keep = keep_ref[...].reshape(parts * rows, double)
    got = got_ref[...].reshape(parts * rows, double)
    total = jnp.dot(keep[:, :width], mine[...], preferred_element_type=F32)
    total = total + jnp.dot(got[:, :width], partner[...], preferred_element_type=F32)
    squares = jnp.sum(keep[:, width:].astype(F32) + got[:, width:].astype(F32), axis=-1, keepdims=True)
    out_ref[:, :, 0:columns] = total.astype(BF16).reshape(parts, rows, columns)
    out_ref[:, :, columns : columns + width] = split(squares, width).reshape(parts, rows, width)


def product(keep, got, mine, partner):
    parts, rows, double = keep.shape
    return pl.pallas_call(
        product_kernel,
        out_shape=jax.ShapeDtypeStruct((parts, rows, mine.shape[1] + double // 2), BF16),
        in_specs=[pl.BlockSpec(memory_space=VMEM)] * 4,
        out_specs=pl.BlockSpec(memory_space=VMEM),
        compiler_params=pltpu.CompilerParams(vmem_limit_bytes=20 << 20),
        name="product",
    )(keep, got, mine, partner)


def finish_kernel(channels, parts_ref, out_ref):
    parts, rows, columns = parts_ref.shape
    wide = out_ref.shape[1]
    squares = jnp.zeros((rows, columns - wide), F32)
    for n in range(parts):
        squares = squares + parts_ref[n, :, wide:columns].astype(F32)
    scale = lax.rsqrt(jnp.sum(squares, axis=-1, keepdims=True) / channels + EPS)
    total = parts_ref[0, :, 0:wide].astype(F32)
    for n in range(1, parts):
        total = total + parts_ref[n, :, 0:wide].astype(F32)
    out_ref[...] = (total * scale).astype(BF16)


def finish(arrived, wide, channels):
    return pl.pallas_call(
        functools.partial(finish_kernel, channels),
        out_shape=jax.ShapeDtypeStruct((arrived.shape[1], wide), BF16),
        in_specs=[pl.BlockSpec(memory_space=VMEM)],
        out_specs=pl.BlockSpec(memory_space=VMEM),
        compiler_params=pltpu.CompilerParams(vmem_limit_bytes=20 << 20),
        name="finish",
    )(arrived)


def ahead(value, steps, first):
    count = lax.axis_size("sp")
    return lax.ppermute(value, "sp", [(source, source + steps) for source in range(first, count - steps)])


def across(value, pairs):
    return lax.ppermute(value, "tp", pairs)


def layer(tokens, norm_gain, w_query, w_key, w_value, out_gain, w_out):
    tok_rows = tokens.shape[0]
    sp = lax.axis_index("sp").astype(jnp.int32).reshape(1)
    tp = lax.axis_index("tp").astype(jnp.int32).reshape(1)
    n_tp = lax.axis_size("tp")
    query, own = qkv(tokens, norm_gain, w_query, w_key, w_value)

    one = ahead(own, 1, 0)
    two = ahead(own, 2, 0)
    three = ahead(two, 1, 2)
    four = ahead(two, 2, 2)
    five = ahead(four, 1, 4)
    excess = 6 * (tok_rows // CLASSES) - WINDOW_THIRD // CLASSES
    six = ahead(four[:, excess:, :], 2, 4)

    swap = [(n, n ^ 1) for n in range(n_tp)]
    same_core = [list(range(core, n_tp, 2)) for core in range(2)]
    partner = across(w_out, swap)
    state = attend_near(sp, query, own, (one, two, three, four))
    keep, give = attend_far(sp, lax.rem(tp, 2), query, five, six, state, out_gain.reshape(1, -1), n_tp // 2)
    got = across(give, swap)
    tiles = product(keep, got, w_out, partner)
    arrived = lax.all_to_all(tiles, "tp", split_axis=0, concat_axis=0, axis_index_groups=same_core, tiled=True)
    return finish(arrived, w_out.shape[1], n_tp * w_out.shape[0])


def solution(mesh):
    in_specs = (
        P(("grp", "sp"), None),
        P(),
        P(None, "tp"),
        P(None, "tp"),
        P(None, "tp"),
        P("tp"),
        P("tp", None),
    )
    out_specs = P(("grp", "sp", "tp"), None)
    return jax.shard_map(layer, mesh=mesh, in_specs=in_specs, out_specs=out_specs, check_vma=False)
```

```python
import functools

import jax
import jax.numpy as jnp
from jax import lax
from jax.experimental import pallas as pl
from jax.experimental.pallas import tpu as pltpu
from jax.sharding import PartitionSpec as P


HEAD_DIM = 64
WINDOW_FIRST = 128
WINDOW_SECOND = 512
DILATION_SECOND = 4
WINDOW_THIRD = 2048
DILATION_THIRD = 16
CLASSES = DILATION_SECOND
EXTRA = 16

EPS = 1e-06
NEG = -1e30


VMEM = pltpu.VMEM
F32 = jnp.float32
BF16 = jnp.bfloat16


def qkv_kernel(
    chunks, tok_hbm, gain_hbm, wq_hbm, wk_hbm, wv_hbm, q_ref, kv_ref, tok, gain_ref, w, acc, gain_sem, tok_sem, w_sem
):
    rows, depth = tok_hbm.shape
    width = wq_hbm.shape[1]
    piece = depth // chunks
    gain_copy = pltpu.make_async_copy(gain_hbm, gain_ref, gain_sem)
    gain_copy.start()
    copies = []
    for n in range(chunks):
        span = pl.ds(n * piece, piece)
        pair = [pltpu.make_async_copy(tok_hbm.at[:, span], tok.at[:, span], tok_sem.at[n])]
        for m, part in enumerate((wq_hbm, wk_hbm, wv_hbm)):
            pair.append(
                pltpu.make_async_copy(
                    part.at[span, :], w.at[span, pl.ds(m * width, width)], w_sem.at[n, m]
                )
            )
        for copy in pair:
            copy.start()
        copies.append(pair)
    gain_copy.wait()
    squares = jnp.zeros((rows, 128), F32)
    for n in range(chunks):
        for copy in copies[n]:
            copy.wait()
        block = tok[:, n * piece : (n + 1) * piece].astype(F32)
        for lane in range(0, piece, 128):
            part = block[:, lane : lane + 128]
            squares = squares + part * part
        tok[:, n * piece : (n + 1) * piece] = (block * gain_ref[:, n * piece : (n + 1) * piece]).astype(BF16)
    total = jnp.dot(tok[...], w[...], preferred_element_type=F32)
    inverse = lax.rsqrt(jnp.sum(squares, axis=-1, keepdims=True) / depth + EPS)
    total = total * inverse
    for m in range(3):
        acc[m] = total[:, m * width : (m + 1) * width]
    share = rows // CLASSES
    for c in range(CLASSES):
        mine = [acc[m, pl.ds(c, share, stride=CLASSES), :] for m in range(3)]
        q_ref[c] = (mine[0] * HEAD_DIM ** (-0.5)).astype(BF16)
        kv_ref[c, :, 0:width] = mine[1].astype(BF16)
        kv_ref[c, :, width : 2 * width] = mine[2].astype(BF16)


def hbm(value):
    return pltpu.with_memory_space_constraint(value, pltpu.HBM)


def qkv(tokens, norm_gain, w_query, w_key, w_value):
    rows, depth = tokens.shape
    width = w_query.shape[1]
    chunks = 2
    share = rows // CLASSES
    return pl.pallas_call(
        functools.partial(qkv_kernel, chunks),
        out_shape=(
            jax.ShapeDtypeStruct((CLASSES, share, width), BF16),
            jax.ShapeDtypeStruct((CLASSES, share, 2 * width), BF16),
        ),
        in_specs=[
            pl.BlockSpec(memory_space=pltpu.HBM),
        ]
        * 5,
        out_specs=(pl.BlockSpec(memory_space=VMEM), pl.BlockSpec(memory_space=VMEM)),
        scratch_shapes=[
            VMEM((rows, depth), BF16),
            VMEM((1, depth), F32),
            VMEM((depth, 3 * width), BF16),
            VMEM((3, rows, width), F32),
            pltpu.SemaphoreType.DMA,
            pltpu.SemaphoreType.DMA((chunks,)),
            pltpu.SemaphoreType.DMA((chunks, 3)),
        ],
        compiler_params=pltpu.CompilerParams(vmem_limit_bytes=20 << 20),
        name="qkv",
    )(hbm(tokens), hbm(norm_gain.reshape(1, depth)), hbm(w_query), hbm(w_key), hbm(w_value))


def split(value, lanes):
    high = value.astype(BF16)
    left = value - high.astype(F32)
    middle = left.astype(BF16)
    low = (left - middle.astype(F32)).astype(BF16)
    lane = lax.broadcasted_iota(jnp.int32, (value.shape[0], lanes), 1)
    zero = jnp.zeros((value.shape[0], lanes), F32)
    spread = jnp.where(lane == 0, high.astype(F32), jnp.where(lane == 1, middle.astype(F32), jnp.where(lane == 2, low.astype(F32), zero)))
    return spread.astype(BF16)


def both_heads(query, lane):
    zero = jnp.zeros_like(query)
    return jnp.concatenate([jnp.where(lane < HEAD_DIM, query, zero), jnp.where(lane < HEAD_DIM, zero, query)], axis=0)


def twice(value):
    return jnp.concatenate([value, value], axis=0)


def third_hit(lag):
    ratio = DILATION_THIRD // CLASSES
    reach = WINDOW_THIRD // CLASSES
    return jnp.logical_and(lag <= reach, lax.rem(lag, ratio) == 0)


CONTRACT = (((1,), (1,)), ((), ()))


def near_kernel(sp_ref, q_ref, own, *rest):
    older = rest[:-5]
    top_ref, norm_ref, sum_ref, k_all, v_all = rest[-5:]
    share, width = q_ref.shape[1:]
    span = k_all.shape[1]
    far = span - share
    near = WINDOW_FIRST // CLASSES
    tail = near + share
    start = span
    for block in (own, *older):
        start -= share
        for c in range(CLASSES):
            k_all[c, start : start + share, :] = block[c, :, 0:width]
            v_all[c, start : start + share, :] = block[c, :, width : 2 * width]
    sp = sp_ref[0]
    row = lax.broadcasted_iota(jnp.int32, (share, span), 0)
    col = lax.broadcasted_iota(jnp.int32, (share, span), 1)
    lag = row - col + far
    behind = lag >= 0
    lag = jnp.maximum(lag, 0)
    count = (
        (lag <= WINDOW_FIRST // CLASSES).astype(F32)
        + (lag <= WINDOW_SECOND // CLASSES).astype(F32)
        + third_hit(lag).astype(F32)
    )
    live = jnp.logical_and(jnp.logical_and(behind, count > 0.5), col >= far - share * sp)
    weight = jnp.where(count > 2.5, jnp.log(F32(3.0)), jnp.where(count > 1.5, jnp.log(F32(2.0)), F32(0.0)))
    bias = twice(jnp.where(live, weight, NEG))
    row = lax.broadcasted_iota(jnp.int32, (share, tail), 0)
    col = lax.broadcasted_iota(jnp.int32, (share, tail), 1)
    lag = row - col + near
    there = col >= near - share * sp
    after = twice(jnp.where(jnp.logical_and(there, jnp.logical_and(lag >= 0, lag < near)), F32(0.0), NEG))
    before = twice(jnp.where(jnp.logical_and(there, jnp.logical_and(lag >= 1, lag <= near)), F32(0.0), NEG))
    lane = lax.broadcasted_iota(jnp.int32, (share, width), 1)
    for c in range(CLASSES):
        stacked = both_heads(q_ref[c], lane)
        scores = [lax.dot_general(stacked, k_all[c], CONTRACT, preferred_element_type=F32) + bias]
        values = [v_all[c]]
        for other in range(CLASSES):
            if other != c:
                part = lax.dot_general(
                    stacked, k_all[other, span - tail : span, :], CONTRACT, preferred_element_type=F32
                )
                scores.append(part + (after if c > other else before))
                values.append(v_all[other, span - tail : span, :])
        top = functools.reduce(jnp.maximum, [jnp.max(part, axis=-1, keepdims=True) for part in scores])
        weights = [jnp.exp(part - top) for part in scores]
        top_ref[c] = top
        norm_ref[c] = functools.reduce(jnp.add, [jnp.sum(part, axis=-1, keepdims=True) for part in weights])
        sum_ref[c] = functools.reduce(
            jnp.add,
            [
                jnp.dot(part.astype(BF16), value, preferred_element_type=F32)
                for part, value in zip(weights, values)
            ],
        )


def attend_near(sp, query, own, older):
    share, width = query.shape[1:]
    span = (1 + len(older)) * share
    return pl.pallas_call(
        near_kernel,
        out_shape=(
            jax.ShapeDtypeStruct((CLASSES, 2 * share, 1), F32),
            jax.ShapeDtypeStruct((CLASSES, 2 * share, 1), F32),
            jax.ShapeDtypeStruct((CLASSES, 2 * share, width), F32),
        ),
        in_specs=[pl.BlockSpec(memory_space=pltpu.SMEM)]
        + [pl.BlockSpec(memory_space=VMEM)] * (2 + len(older)),
        out_specs=(pl.BlockSpec(memory_space=VMEM),) * 3,
        scratch_shapes=[VMEM((CLASSES, span, width), BF16), VMEM((CLASSES, span, width), BF16)],
        compiler_params=pltpu.CompilerParams(vmem_limit_bytes=20 << 20),
        name="attend_near",
    )(sp, query, own, *older)


def far_kernel(sp_ref, core_ref, q_ref, five, six, top_ref, norm_ref, sum_ref, gain_ref, keep_ref, give_ref, natural):
    share, width = q_ref.shape[1:]
    count = five.shape[1] + six.shape[1]
    far = WINDOW_THIRD // CLASSES
    row = lax.broadcasted_iota(jnp.int32, (share, count), 0)
    col = lax.broadcasted_iota(jnp.int32, (share, count), 1)
    live = jnp.logical_and(third_hit(row - col + far), col >= far - share * sp_ref[0])
    bias = twice(jnp.where(live, F32(0.0), NEG))
    lane = lax.broadcasted_iota(jnp.int32, (share, width), 1)
    for c in range(CLASSES):
        stacked = both_heads(q_ref[c], lane)
        keys = jnp.concatenate([six[c, :, 0:width], five[c, :, 0:width]], axis=0)
        values = jnp.concatenate([six[c, :, width : 2 * width], five[c, :, width : 2 * width]], axis=0)
        score = lax.dot_general(stacked, keys, CONTRACT, preferred_element_type=F32) + bias
        top = jnp.maximum(top_ref[c], jnp.max(score, axis=-1, keepdims=True))
        shrink = jnp.exp(top_ref[c] - top)
        weight = jnp.exp(score - top)
        norm = norm_ref[c] * shrink + jnp.sum(weight, axis=-1, keepdims=True)
        mixed = sum_ref[c] * shrink + jnp.dot(weight.astype(BF16), values, preferred_element_type=F32)
        mixed = mixed / norm
        natural[pl.ds(c, share, stride=CLASSES), :] = jnp.where(lane < HEAD_DIM, mixed[:share], mixed[share:])
    core = core_ref[0]
    part = keep_ref.shape[1]
    for side, target in ((core, keep_ref), (1 - core, give_ref)):
        for place in range(keep_ref.shape[0]):
            first = pl.multiple_of((2 * place + side) * part, 16)
            block = natural[pl.ds(first, part), :]
            target[place, :, 0:width] = (block * gain_ref[...]).astype(BF16)
            target[place, :, width : 2 * width] = split(jnp.sum(block * block, axis=-1, keepdims=True), width)


def attend_far(sp, core, query, five, six, state, gain, parts):
    share, width = query.shape[1:]
    return pl.pallas_call(
        far_kernel,
        out_shape=(jax.ShapeDtypeStruct((parts, CLASSES * share // (2 * parts), 2 * width), BF16),) * 2,
        in_specs=[pl.BlockSpec(memory_space=pltpu.SMEM)] * 2 + [pl.BlockSpec(memory_space=VMEM)] * 7,
        out_specs=(pl.BlockSpec(memory_space=VMEM),) * 2,
        scratch_shapes=[VMEM((CLASSES * share, width), F32)],
        compiler_params=pltpu.CompilerParams(vmem_limit_bytes=20 << 20),
        name="attend_far",
    )(sp, core, query, five, six, *state, gain)


def turned(column_or_row, rows, axis):
    shape = (rows, 128)
    same = lax.broadcasted_iota(jnp.int32, shape, 0) == lax.broadcasted_iota(jnp.int32, shape, 1)
    return jnp.sum(jnp.where(same, column_or_row, F32(0.0)), axis=axis, keepdims=True)


def product_kernel(keep_ref, got_ref, mine, partner, out_ref):
    parts, rows, double = keep_ref.shape
    width = double // 2
    columns = mine.shape[1]
    keep = keep_ref[...].reshape(parts * rows, double)
    got = got_ref[...].reshape(parts * rows, double)
    total = jnp.dot(keep[:, :width], mine[...], preferred_element_type=F32)
    total = total + jnp.dot(got[:, :width], partner[...], preferred_element_type=F32)
    squares = jnp.sum(keep[:, width:].astype(F32) + got[:, width:].astype(F32), axis=-1, keepdims=True)
    below = rows * columns // 128
    line = lax.broadcasted_iota(jnp.int32, (EXTRA, 128), 0)
    for place in range(parts):
        mine_rows = slice(place * rows, (place + 1) * rows)
        for n in range(columns // 128):
            out_ref[place, n * rows : (n + 1) * rows, :] = total[mine_rows, n * 128 : (n + 1) * 128].astype(BF16)
        whole = turned(squares[mine_rows], rows, 0)
        high = whole.astype(BF16).astype(F32)
        middle = (whole - high).astype(BF16).astype(F32)
        low = whole - high - middle
        extra = jnp.where(line == 0, high, jnp.where(line == 1, middle, jnp.where(line == 2, low, F32(0.0))))
        out_ref[place, below : below + EXTRA, :] = extra.astype(BF16)


def product(keep, got, mine, partner):
    parts, rows, _ = keep.shape
    return pl.pallas_call(
        product_kernel,
        out_shape=jax.ShapeDtypeStruct((parts, rows * mine.shape[1] // 128 + EXTRA, 128), BF16),
        in_specs=[pl.BlockSpec(memory_space=VMEM)] * 4,
        out_specs=pl.BlockSpec(memory_space=VMEM),
        compiler_params=pltpu.CompilerParams(vmem_limit_bytes=20 << 20),
        name="product",
    )(keep, got, mine, partner)


def finish_kernel(channels, parts_ref, out_ref):
    parts = parts_ref.shape[0]
    rows, columns = out_ref.shape
    below = rows * columns // 128
    squares = functools.reduce(
        jnp.add, [parts_ref[place, below : below + EXTRA, :].astype(F32) for place in range(parts)]
    )
    squares = turned(jnp.sum(squares, axis=0, keepdims=True), rows, 1)
    scale = lax.rsqrt(squares / channels + EPS)
    for n in range(columns // 128):
        total = functools.reduce(
            jnp.add, [parts_ref[place, n * rows : (n + 1) * rows, :].astype(F32) for place in range(parts)]
        )
        out_ref[:, n * 128 : (n + 1) * 128] = (total * scale).astype(BF16)


def finish(arrived, rows, wide, channels):
    return pl.pallas_call(
        functools.partial(finish_kernel, channels),
        out_shape=jax.ShapeDtypeStruct((rows, wide), BF16),
        in_specs=[pl.BlockSpec(memory_space=VMEM)],
        out_specs=pl.BlockSpec(memory_space=VMEM),
        compiler_params=pltpu.CompilerParams(vmem_limit_bytes=20 << 20),
        name="finish",
    )(arrived)


def ahead(value, steps, first):
    count = lax.axis_size("sp")
    return lax.ppermute(value, "sp", [(source, source + steps) for source in range(first, count - steps)])


def across(value, pairs):
    return lax.ppermute(value, "tp", pairs)


def layer(tokens, norm_gain, w_query, w_key, w_value, out_gain, w_out):
    tok_rows = tokens.shape[0]
    sp = lax.axis_index("sp").astype(jnp.int32).reshape(1)
    tp = lax.axis_index("tp").astype(jnp.int32).reshape(1)
    n_tp = lax.axis_size("tp")
    query, own = qkv(tokens, norm_gain, w_query, w_key, w_value)

    one = ahead(own, 1, 0)
    two = ahead(own, 2, 0)
    three = ahead(two, 1, 2)
    four = ahead(two, 2, 2)
    five = ahead(four, 1, 4)
    excess = 6 * (tok_rows // CLASSES) - WINDOW_THIRD // CLASSES
    six = ahead(four[:, excess:, :], 2, 4)

    swap = [(n, n ^ 1) for n in range(n_tp)]
    same_core = [list(range(core, n_tp, 2)) for core in range(2)]
    partner = across(w_out, swap)
    state = attend_near(sp, query, own, (one, two, three, four))
    keep, give = attend_far(sp, lax.rem(tp, 2), query, five, six, state, out_gain.reshape(1, -1), n_tp // 2)
    got = across(give, swap)
    tiles = product(keep, got, w_out, partner)
    arrived = lax.all_to_all(tiles, "tp", split_axis=0, concat_axis=0, axis_index_groups=same_core, tiled=True)
    return finish(arrived, tok_rows // n_tp, w_out.shape[1], n_tp * w_out.shape[0])


def solution(mesh):
    in_specs = (
        P(("grp", "sp"), None),
        P(),
        P(None, "tp"),
        P(None, "tp"),
        P(None, "tp"),
        P("tp"),
        P("tp", None),
    )
    out_specs = P(("grp", "sp", "tp"), None)
    return jax.shard_map(layer, mesh=mesh, in_specs=in_specs, out_specs=out_specs, check_vma=False)
```

```python
import functools

import jax
import jax.numpy as jnp
from jax import lax
from jax.experimental import pallas as pl
from jax.experimental.pallas import tpu as pltpu
from jax.sharding import PartitionSpec as P


HEAD_DIM = 64
WINDOW_FIRST = 128
WINDOW_SECOND = 512
DILATION_SECOND = 4
WINDOW_THIRD = 2048
DILATION_THIRD = 16
CLASSES = DILATION_SECOND
EXTRA = 16

EPS = 1e-06
NEG = -1e30


VMEM = pltpu.VMEM
F32 = jnp.float32
BF16 = jnp.bfloat16


def qkv_kernel(
    chunks, tok_hbm, gain_hbm, wq_hbm, wk_hbm, wv_hbm, q_ref, kv_ref, tok, gain_ref, w, acc, gain_sem, tok_sem, w_sem
):
    rows, depth = tok_hbm.shape
    width = wq_hbm.shape[1]
    piece = depth // chunks
    gain_copy = pltpu.make_async_copy(gain_hbm, gain_ref, gain_sem)
    gain_copy.start()
    copies = []
    for n in range(chunks):
        span = pl.ds(n * piece, piece)
        pair = [pltpu.make_async_copy(tok_hbm.at[:, span], tok.at[:, span], tok_sem.at[n])]
        for m, part in enumerate((wq_hbm, wk_hbm, wv_hbm)):
            pair.append(
                pltpu.make_async_copy(
                    part.at[span, :], w.at[span, pl.ds(m * width, width)], w_sem.at[n, m]
                )
            )
        for copy in pair:
            copy.start()
        copies.append(pair)
    gain_copy.wait()
    squares = jnp.zeros((rows, 128), F32)
    for n in range(chunks):
        for copy in copies[n]:
            copy.wait()
        block = tok[:, n * piece : (n + 1) * piece].astype(F32)
        for lane in range(0, piece, 128):
            part = block[:, lane : lane + 128]
            squares = squares + part * part
        tok[:, n * piece : (n + 1) * piece] = (block * gain_ref[:, n * piece : (n + 1) * piece]).astype(BF16)
    total = jnp.dot(tok[...], w[...], preferred_element_type=F32)
    inverse = lax.rsqrt(jnp.sum(squares, axis=-1, keepdims=True) / depth + EPS)
    total = total * inverse
    for m in range(3):
        acc[m] = total[:, m * width : (m + 1) * width]
    share = rows // CLASSES
    for c in range(CLASSES):
        mine = [acc[m, pl.ds(c, share, stride=CLASSES), :] for m in range(3)]
        q_ref[c] = (mine[0] * HEAD_DIM ** (-0.5)).astype(BF16)
        kv_ref[c, :, 0:width] = mine[1].astype(BF16)
        kv_ref[c, :, width : 2 * width] = mine[2].astype(BF16)


def hbm(value):
    return pltpu.with_memory_space_constraint(value, pltpu.HBM)


def qkv(tokens, norm_gain, w_query, w_key, w_value):
    rows, depth = tokens.shape
    width = w_query.shape[1]
    chunks = 2
    share = rows // CLASSES
    return pl.pallas_call(
        functools.partial(qkv_kernel, chunks),
        out_shape=(
            jax.ShapeDtypeStruct((CLASSES, share, width), BF16),
            jax.ShapeDtypeStruct((CLASSES, share, 2 * width), BF16),
        ),
        in_specs=[
            pl.BlockSpec(memory_space=pltpu.HBM),
        ]
        * 5,
        out_specs=(pl.BlockSpec(memory_space=VMEM), pl.BlockSpec(memory_space=VMEM)),
        scratch_shapes=[
            VMEM((rows, depth), BF16),
            VMEM((1, depth), F32),
            VMEM((depth, 3 * width), BF16),
            VMEM((3, rows, width), F32),
            pltpu.SemaphoreType.DMA,
            pltpu.SemaphoreType.DMA((chunks,)),
            pltpu.SemaphoreType.DMA((chunks, 3)),
        ],
        compiler_params=pltpu.CompilerParams(vmem_limit_bytes=20 << 20),
        name="qkv",
    )(hbm(tokens), hbm(norm_gain.reshape(1, depth)), hbm(w_query), hbm(w_key), hbm(w_value))


def split(value, lanes):
    high = value.astype(BF16)
    left = value - high.astype(F32)
    middle = left.astype(BF16)
    low = (left - middle.astype(F32)).astype(BF16)
    lane = lax.broadcasted_iota(jnp.int32, (value.shape[0], lanes), 1)
    zero = jnp.zeros((value.shape[0], lanes), F32)
    spread = jnp.where(lane == 0, high.astype(F32), jnp.where(lane == 1, middle.astype(F32), jnp.where(lane == 2, low.astype(F32), zero)))
    return spread.astype(BF16)


def both_heads(query, lane):
    zero = jnp.zeros_like(query)
    return jnp.concatenate([jnp.where(lane < HEAD_DIM, query, zero), jnp.where(lane < HEAD_DIM, zero, query)], axis=0)


def twice(value):
    return jnp.concatenate([value, value], axis=0)


def third_hit(lag):
    ratio = DILATION_THIRD // CLASSES
    reach = WINDOW_THIRD // CLASSES
    return jnp.logical_and(lag <= reach, lax.rem(lag, ratio) == 0)


CONTRACT = (((1,), (1,)), ((), ()))


def near_kernel(sp_ref, q_ref, own, *rest):
    older = rest[:-5]
    top_ref, norm_ref, sum_ref, k_all, v_all = rest[-5:]
    share, width = q_ref.shape[1:]
    span = k_all.shape[1]
    far = span - share
    near = WINDOW_FIRST // CLASSES
    tail = near + share
    start = span
    for block in (own, *older):
        start -= share
        for c in range(CLASSES):
            k_all[c, start : start + share, :] = block[c, :, 0:width]
            v_all[c, start : start + share, :] = block[c, :, width : 2 * width]
    sp = sp_ref[0]
    row = lax.broadcasted_iota(jnp.int32, (share, span), 0)
    col = lax.broadcasted_iota(jnp.int32, (share, span), 1)
    lag = row - col + far
    behind = lag >= 0
    lag = jnp.maximum(lag, 0)
    count = (
        (lag <= WINDOW_FIRST // CLASSES).astype(F32)
        + (lag <= WINDOW_SECOND // CLASSES).astype(F32)
        + third_hit(lag).astype(F32)
    )
    live = jnp.logical_and(jnp.logical_and(behind, count > 0.5), col >= far - share * sp)
    weight = jnp.where(count > 2.5, jnp.log(F32(3.0)), jnp.where(count > 1.5, jnp.log(F32(2.0)), F32(0.0)))
    bias = twice(jnp.where(live, weight, NEG))
    row = lax.broadcasted_iota(jnp.int32, (share, tail), 0)
    col = lax.broadcasted_iota(jnp.int32, (share, tail), 1)
    lag = row - col + near
    there = col >= near - share * sp
    after = twice(jnp.where(jnp.logical_and(there, jnp.logical_and(lag >= 0, lag < near)), F32(0.0), NEG))
    before = twice(jnp.where(jnp.logical_and(there, jnp.logical_and(lag >= 1, lag <= near)), F32(0.0), NEG))
    lane = lax.broadcasted_iota(jnp.int32, (share, width), 1)
    for c in range(CLASSES):
        stacked = both_heads(q_ref[c], lane)
        scores = [lax.dot_general(stacked, k_all[c], CONTRACT, preferred_element_type=F32) + bias]
        values = [v_all[c]]
        for other in range(CLASSES):
            if other != c:
                part = lax.dot_general(
                    stacked, k_all[other, span - tail : span, :], CONTRACT, preferred_element_type=F32
                )
                scores.append(part + (after if c > other else before))
                values.append(v_all[other, span - tail : span, :])
        top = functools.reduce(jnp.maximum, [jnp.max(part, axis=-1, keepdims=True) for part in scores])
        weights = [jnp.exp(part - top) for part in scores]
        top_ref[c] = top
        norm_ref[c] = functools.reduce(jnp.add, [jnp.sum(part, axis=-1, keepdims=True) for part in weights])
        sum_ref[c] = functools.reduce(
            jnp.add,
            [
                jnp.dot(part.astype(BF16), value, preferred_element_type=F32)
                for part, value in zip(weights, values)
            ],
        )


def attend_near(sp, query, own, older):
    share, width = query.shape[1:]
    span = (1 + len(older)) * share
    return pl.pallas_call(
        near_kernel,
        out_shape=(
            jax.ShapeDtypeStruct((CLASSES, 2 * share, 1), F32),
            jax.ShapeDtypeStruct((CLASSES, 2 * share, 1), F32),
            jax.ShapeDtypeStruct((CLASSES, 2 * share, width), F32),
        ),
        in_specs=[pl.BlockSpec(memory_space=pltpu.SMEM)]
        + [pl.BlockSpec(memory_space=VMEM)] * (2 + len(older)),
        out_specs=(pl.BlockSpec(memory_space=VMEM),) * 3,
        scratch_shapes=[VMEM((CLASSES, span, width), BF16), VMEM((CLASSES, span, width), BF16)],
        compiler_params=pltpu.CompilerParams(vmem_limit_bytes=20 << 20),
        name="attend_near",
    )(sp, query, own, *older)


def far_kernel(sp_ref, core_ref, q_ref, *rest):
    blocks = rest[:-7]
    top_ref, norm_ref, sum_ref, gain_ref, keep_ref, give_ref, natural = rest[-7:]
    share, width = q_ref.shape[1:]
    count = sum(block.shape[1] for block in blocks)
    far = WINDOW_THIRD // CLASSES
    row = lax.broadcasted_iota(jnp.int32, (share, count), 0)
    col = lax.broadcasted_iota(jnp.int32, (share, count), 1)
    live = jnp.logical_and(third_hit(row - col + far), col >= far - share * sp_ref[0])
    bias = twice(jnp.where(live, F32(0.0), NEG))
    lane = lax.broadcasted_iota(jnp.int32, (share, width), 1)
    for c in range(CLASSES):
        stacked = both_heads(q_ref[c], lane)
        keys = jnp.concatenate([block[c, :, 0:width] for block in blocks[::-1]], axis=0)
        values = jnp.concatenate([block[c, :, width : 2 * width] for block in blocks[::-1]], axis=0)
        score = lax.dot_general(stacked, keys, CONTRACT, preferred_element_type=F32) + bias
        top = jnp.maximum(top_ref[c], jnp.max(score, axis=-1, keepdims=True))
        shrink = jnp.exp(top_ref[c] - top)
        weight = jnp.exp(score - top)
        norm = norm_ref[c] * shrink + jnp.sum(weight, axis=-1, keepdims=True)
        mixed = sum_ref[c] * shrink + jnp.dot(weight.astype(BF16), values, preferred_element_type=F32)
        mixed = mixed / norm
        natural[pl.ds(c, share, stride=CLASSES), :] = jnp.where(lane < HEAD_DIM, mixed[:share], mixed[share:])
    core = core_ref[0]
    part = keep_ref.shape[1]
    for side, target in ((core, keep_ref), (1 - core, give_ref)):
        for place in range(keep_ref.shape[0]):
            first = pl.multiple_of((2 * place + side) * part, 16)
            block = natural[pl.ds(first, part), :]
            target[place, :, 0:width] = (block * gain_ref[...]).astype(BF16)
            target[place, :, width : 2 * width] = split(jnp.sum(block * block, axis=-1, keepdims=True), width)


def attend_far(sp, core, query, blocks, state, gain, parts):
    share, width = query.shape[1:]
    return pl.pallas_call(
        far_kernel,
        out_shape=(jax.ShapeDtypeStruct((parts, CLASSES * share // (2 * parts), 2 * width), BF16),) * 2,
        in_specs=[pl.BlockSpec(memory_space=pltpu.SMEM)] * 2 + [pl.BlockSpec(memory_space=VMEM)] * (5 + len(blocks)),
        out_specs=(pl.BlockSpec(memory_space=VMEM),) * 2,
        scratch_shapes=[VMEM((CLASSES * share, width), F32)],
        compiler_params=pltpu.CompilerParams(vmem_limit_bytes=20 << 20),
        name="attend_far",
    )(sp, core, query, *blocks, *state, gain)


def turned(column_or_row, rows, axis):
    shape = (rows, 128)
    same = lax.broadcasted_iota(jnp.int32, shape, 0) == lax.broadcasted_iota(jnp.int32, shape, 1)
    return jnp.sum(jnp.where(same, column_or_row, F32(0.0)), axis=axis, keepdims=True)


def product_kernel(keep_ref, got_ref, mine, partner, out_ref):
    parts, rows, double = keep_ref.shape
    width = double // 2
    columns = mine.shape[1]
    keep = keep_ref[...].reshape(parts * rows, double)
    got = got_ref[...].reshape(parts * rows, double)
    total = jnp.dot(keep[:, :width], mine[...], preferred_element_type=F32)
    total = total + jnp.dot(got[:, :width], partner[...], preferred_element_type=F32)
    squares = jnp.sum(keep[:, width:].astype(F32) + got[:, width:].astype(F32), axis=-1, keepdims=True)
    below = rows * columns // 128
    line = lax.broadcasted_iota(jnp.int32, (EXTRA, 128), 0)
    for place in range(parts):
        mine_rows = slice(place * rows, (place + 1) * rows)
        for n in range(columns // 128):
            out_ref[place, n * rows : (n + 1) * rows, :] = total[mine_rows, n * 128 : (n + 1) * 128].astype(BF16)
        whole = turned(squares[mine_rows], rows, 0)
        high = whole.astype(BF16).astype(F32)
        middle = (whole - high).astype(BF16).astype(F32)
        low = whole - high - middle
        extra = jnp.where(line == 0, high, jnp.where(line == 1, middle, jnp.where(line == 2, low, F32(0.0))))
        out_ref[place, below : below + EXTRA, :] = extra.astype(BF16)


def product(keep, got, mine, partner):
    parts, rows, _ = keep.shape
    return pl.pallas_call(
        product_kernel,
        out_shape=jax.ShapeDtypeStruct((parts, rows * mine.shape[1] // 128 + EXTRA, 128), BF16),
        in_specs=[pl.BlockSpec(memory_space=VMEM)] * 4,
        out_specs=pl.BlockSpec(memory_space=VMEM),
        compiler_params=pltpu.CompilerParams(vmem_limit_bytes=20 << 20),
        name="product",
    )(keep, got, mine, partner)


def finish_kernel(channels, parts_ref, out_ref):
    parts = parts_ref.shape[0]
    rows, columns = out_ref.shape
    below = rows * columns // 128
    squares = functools.reduce(
        jnp.add, [parts_ref[place, below : below + EXTRA, :].astype(F32) for place in range(parts)]
    )
    squares = turned(jnp.sum(squares, axis=0, keepdims=True), rows, 1)
    scale = lax.rsqrt(squares / channels + EPS)
    for n in range(columns // 128):
        total = functools.reduce(
            jnp.add, [parts_ref[place, n * rows : (n + 1) * rows, :].astype(F32) for place in range(parts)]
        )
        out_ref[:, n * 128 : (n + 1) * 128] = (total * scale).astype(BF16)


def finish(arrived, rows, wide, channels):
    return pl.pallas_call(
        functools.partial(finish_kernel, channels),
        out_shape=jax.ShapeDtypeStruct((rows, wide), BF16),
        in_specs=[pl.BlockSpec(memory_space=VMEM)],
        out_specs=pl.BlockSpec(memory_space=VMEM),
        compiler_params=pltpu.CompilerParams(vmem_limit_bytes=20 << 20),
        name="finish",
    )(arrived)


def ahead(value, steps, first):
    count = lax.axis_size("sp")
    return lax.ppermute(value, "sp", [(source, source + steps) for source in range(first, count - steps)])


def across(value, pairs):
    return lax.ppermute(value, "tp", pairs)


def layer(tokens, norm_gain, w_query, w_key, w_value, out_gain, w_out):
    tok_rows = tokens.shape[0]
    sp = lax.axis_index("sp").astype(jnp.int32).reshape(1)
    tp = lax.axis_index("tp").astype(jnp.int32).reshape(1)
    n_tp = lax.axis_size("tp")
    query, own = qkv(tokens, norm_gain, w_query, w_key, w_value)

    one = ahead(own, 1, 0)
    two = ahead(own, 2, 0)
    three = ahead(two, 1, 2)
    four = ahead(two, 2, 2)
    five = ahead(four, 1, 4)
    excess = 6 * (tok_rows // CLASSES) - WINDOW_THIRD // CLASSES
    six = ahead(four[:, excess:, :], 2, 4)

    swap = [(n, n ^ 1) for n in range(n_tp)]
    same_core = [list(range(core, n_tp, 2)) for core in range(2)]
    partner = across(w_out, swap)
    state = attend_near(sp, query, own, (one, two))
    far = (three, four, five, six)
    keep, give = attend_far(sp, lax.rem(tp, 2), query, far, state, out_gain.reshape(1, -1), n_tp // 2)
    got = across(give, swap)
    tiles = product(keep, got, w_out, partner)
    arrived = lax.all_to_all(tiles, "tp", split_axis=0, concat_axis=0, axis_index_groups=same_core, tiled=True)
    return finish(arrived, tok_rows // n_tp, w_out.shape[1], n_tp * w_out.shape[0])


def solution(mesh):
    in_specs = (
        P(("grp", "sp"), None),
        P(),
        P(None, "tp"),
        P(None, "tp"),
        P(None, "tp"),
        P("tp"),
        P("tp", None),
    )
    out_specs = P(("grp", "sp", "tp"), None)
    return jax.shard_map(layer, mesh=mesh, in_specs=in_specs, out_specs=out_specs, check_vma=False)
```
